32 devices in a mesh: sp: 8 (over z, x), tp: 4 (over y, core).
Axes of the slice: x: 2, y: 2, z: 4, core: 2. Of those that a mesh axis runs over, the one named last changes fastest.
Arguments:
- queries: bfloat16 [3072, 768], P('sp', 'tp'), may hold values from -8 to 8
- keys: bfloat16 [3072, 256], P('sp', 'tp'), may hold values from -8 to 8
- values: bfloat16 [3072, 256], P('sp', 'tp'), may hold values from -6 to 6
- sinks: float32 [12], P('tp'), may hold values from 1 to 6
- residual: bfloat16 [3072, 2048], P('sp'), may hold values from -6 to 6
- out_weight: bfloat16 [768, 2048], replicated, may hold values from -3 to 3
- norm_gain: float32 [2048], replicated, may hold values from 0.1 to 1.9
- shared_gate: bfloat16 [2048, 512], P(None, 'tp'), may hold values from -0.125 to 0.125
- shared_up: bfloat16 [2048, 512], P(None, 'tp'), may hold values from -0.125 to 0.125
- shared_down: bfloat16 [512, 2048], P('tp'), may hold values from -0.25 to 0.25
- expert_ids: int32 [3072, 2], P('sp'), may hold values from 0 to 15, all different within a row; in each aligned block of 96 rows (0 to 95, 96 to 191, ...) at most 24 rows name the same one
- route_weights: float32 [3072, 2], P(('sp', 'tp')), may hold values from 0.2 to 2
- expert_gate: bfloat16 [16, 2048, 1024], P('sp', None, 'tp'), may hold values from -0.125 to 0.125
- expert_up: bfloat16 [16, 2048, 1024], P('sp', None, 'tp'), may hold values from -0.125 to 0.125
- expert_down: bfloat16 [16, 1024, 2048], P('sp', 'tp'), may hold values from -0.1875 to 0.1875
Outputs:
- layer_out: bfloat16 [3072, 2048], P(('sp', 'tp'))
The draws below stay inside these ranges and needn't reach their ends.
Inputs may be any that keep to these rules, and one draw needn't show every extreme that they name: `expert_ids`: each row names 2 different experts. In each aligned block of 96 rows no expert is named more than 24 times, a bound that some blocks reach.
All inputs are finite; a program needn't handle non-finite values.
Results may differ from the reference program's by a relative error of at most 0.018.
Values may be sent and summed in bfloat16 or wider, within the bound.
A program may use at most 128 MiB of HBM per device.

```python
import math
import jax
import jax.numpy as jnp
import numpy as np
from jax import lax

D = 2048
HEADS = 12
KV_HEADS = 4
HEAD_DIM = 64
WINDOW = 128
GRID_W = 64
EXP_HID = 1024
SHARED_HID = 512
TOPK = 2
TOKENS = 3072
OWN = 96
EXPERTS = 16
CAP = 24
N_TP = 4


def drawn_pair(key):
    seeded = jax.random.fold_in(key, 7)
    query_seed, key_seed = jax.random.split(seeded, 2)
    queries = jnp.clip(jax.random.normal(query_seed, (TOKENS, HEADS, HEAD_DIM), jnp.float32), -6.0, 6.0)
    keys = jnp.clip(jax.random.normal(key_seed, (TOKENS, KV_HEADS, HEAD_DIM), jnp.float32), -6.0, 6.0)
    return (queries.reshape(TOKENS, HEADS * HEAD_DIM), keys.reshape(TOKENS, KV_HEADS * HEAD_DIM))


def draw_queries(key, part):
    return drawn_pair(key)[0].astype(jnp.bfloat16)


def draw_keys(key, part):
    return drawn_pair(key)[1].astype(jnp.bfloat16)


def shard_levels(own_key, dims, shards, low, largest):
    def one(position, shards_of):
        draws = jax.random.uniform(jax.random.fold_in(jax.random.fold_in(own_key, 6), position), (shards_of,), jnp.float32, low / len(shards), largest / len(shards))
        return jnp.repeat(jnp.exp(draws), dims[position] // shards_of).reshape((-1,) + (1,) * (len(dims) - position - 1))

    loudness = one(*shards[0])
    for cut in shards[1:]:
        loudness = loudness * one(*cut)
    return loudness


def assign_block(rng, own, number, rows, amount, top, bound, slope):
    sequence = jax.random.permutation(rng, amount)
    packed, usual = portions_of(amount, rows * top, bound, slope, True), portions_of(amount, rows * top, bound, slope, False)
    places = jnp.arange(amount)

    def named(tallies, turn):
        used = int((tallies > 0).sum())
        fixed = max(1, used // 4)
        moved = fixed + (places - fixed + turn * (used - fixed)) % max(1, amount - fixed)
        return jnp.zeros((amount,), jnp.int32).at[sequence[jnp.where(places < fixed, places, moved)]].set(jnp.asarray(tallies, jnp.int32))

    tallies = jnp.where(number % 4 == 0, named(packed, number // 4), named(usual, number - number // 4 - 1))
    mixed = jax.random.permutation(jax.random.fold_in(own, 3), amount)
    source_of, receiver = mixed[0:amount // 2 * 2:2], mixed[1:amount // 2 * 2:2]
    room = jnp.minimum(tallies[source_of] - 1, bound - tallies[receiver]) // 2
    room = jnp.where((source_of == sequence[0]) | (receiver == sequence[0]) | (tallies[receiver] == 0), 0, jnp.maximum(room, 0))
    moved = jax.random.randint(jax.random.fold_in(own, 4), (amount // 2,), 0, 1 << 20) % (room + 1)
    tallies = tallies.at[source_of].add(-moved).at[receiver].add(moved)
    items = jnp.searchsorted(jnp.cumsum(tallies), jnp.arange(rows * top), side="right").astype(jnp.int32)
    listing = items.reshape(top, rows).T
    listing = listing[jax.random.permutation(jax.random.fold_in(own, 1), rows)]
    turn = jax.random.randint(jax.random.fold_in(own, 2), (rows, 1), 0, top)
    return jnp.take_along_axis(listing, (jnp.arange(top)[None, :] + turn) % top, axis=1)


def portions_of(amount, total, most, slope, full):
    portions = [(1 << 20) // math.isqrt(rank ** slope) + 1 for rank in range(1, amount + 1)]
    largest = most if full else min(most, max(-(-total // amount), total * portions[0] // sum(portions)))
    least = 1 if total - largest >= amount - 1 else 0
    counts, surplus = [largest] + [least] * (amount - 1), total - largest - least * (amount - 1)
    while surplus > 0:
        free = [i for i in range(1, amount) if counts[i] < largest] or [i for i in range(1, amount) if counts[i] < most]
        pool, budget = sum([portions[i] for i in free]), surplus
        for i in free:
            more = min(most - counts[i], max(1, budget * portions[i] // pool), surplus)
            counts[i] = counts[i] + more
            surplus = surplus - more
    return np.array(counts)


def centred(rng, shape, width, limit, cuts=(), kind=jnp.bfloat16):
    gain = shard_levels(rng, shape, cuts, -0.22, 0.18) if cuts else 1.0
    values = jax.random.normal(rng, shape, jnp.float32) * width * gain
    return jnp.minimum(jnp.maximum(values, -limit), limit).astype(kind)


def setup_inputs(seed: int = 0) -> dict:
    arg_keys = jax.random.split(jax.random.key(seed), 16)
    queries = draw_queries(jax.random.fold_in(arg_keys[15], 71), 0)
    keys = draw_keys(jax.random.fold_in(arg_keys[15], 71), 0)
    values = centred(arg_keys[2], (TOKENS, KV_HEADS * HEAD_DIM), 1.0, 6.0, ((0, 8), (1, 4)))
    sinks = jnp.clip(1.0 + 5.0 * jax.random.uniform(arg_keys[3], (HEADS,), jnp.float32) ** shard_levels(arg_keys[3], (HEADS,), ((0, 4),), -0.2, 0.2), 1.0, 6.0)
    residual = centred(arg_keys[4], (TOKENS, D), 1.0, 6.0, ((0, 8),))
    out_weight = centred(arg_keys[5], (HEADS * HEAD_DIM, D), 0.5, 3.0)
    norm_gain = jnp.clip(1.0 + 0.18 * jax.random.normal(arg_keys[6], (D,), jnp.float32), 0.1, 1.9)
    shared_gate = centred(arg_keys[7], (D, SHARED_HID), D ** -0.5, 0.125, ((1, 4),))
    shared_up = centred(arg_keys[8], (D, SHARED_HID), D ** -0.5, 0.125, ((1, 4),))
    shared_down = centred(arg_keys[9], (SHARED_HID, D), SHARED_HID ** -0.5, 0.25, ((0, 4),))
    expert_ids_keys = jax.random.split(jax.random.fold_in(arg_keys[10], 1), TOKENS // OWN)
    expert_ids_turns = jax.random.permutation(jax.random.fold_in(arg_keys[10], 3), TOKENS // OWN)
    expert_ids = jax.vmap(lambda own, number: assign_block(jax.random.fold_in(arg_keys[10], 2), own, number, OWN, EXPERTS, TOPK, CAP, 2))(expert_ids_keys, expert_ids_turns).reshape((TOKENS, TOPK))
    route_weights = jnp.clip(jnp.exp(math.log(2.0) - 2.3025851 * jax.random.uniform(arg_keys[11], (TOKENS, TOPK), jnp.float32) ** shard_levels(arg_keys[11], (TOKENS, TOPK), ((0, 32),), -0.2, 0.2)), 0.2, 2.0)
    expert_gate = centred(arg_keys[12], (EXPERTS, D, EXP_HID), D ** -0.5, 0.125, ((0, 8), (2, 4)))
    expert_up = centred(arg_keys[13], (EXPERTS, D, EXP_HID), D ** -0.5, 0.125, ((0, 8), (2, 4)))
    expert_down = centred(arg_keys[14], (EXPERTS, EXP_HID, D), EXP_HID ** -0.5, 0.1875, ((0, 8), (1, 4)))
    return {"queries": queries, "keys": keys, "values": values, "sinks": sinks, "residual": residual, "out_weight": out_weight, "norm_gain": norm_gain, "shared_gate": shared_gate, "shared_up": shared_up, "shared_down": shared_down, "expert_ids": expert_ids, "route_weights": route_weights, "expert_gate": expert_gate, "expert_up": expert_up, "expert_down": expert_down}


ROPE_BASE = 10000.0
NEG_LARGE = -1e+30
NORM_EPSILON = 1e-06

def rotary_turn(values, places, turn_sign):
    halfway = values.shape[-1] // 2
    quarter = halfway // 2
    spectrum = ROPE_BASE ** (-jnp.arange(0, halfway, 2, dtype=jnp.float32) / halfway)

    def rotate_by(segment, offsets_at):
        angles = turn_sign * offsets_at.astype(jnp.float32)[:, None] * spectrum[None, :]
        cosine = jnp.cos(angles)[:, None, :]
        sine_part = jnp.sin(angles)[:, None, :]
        former = segment[..., :quarter]
        latter = segment[..., quarter:]
        return jnp.concatenate([former * cosine - latter * sine_part, former * sine_part + latter * cosine], axis=-1)
    return jnp.concatenate([rotate_by(values[..., :halfway], places // GRID_W), rotate_by(values[..., halfway:], places % GRID_W)], axis=-1)

def attend(queries, keys, values, sinks):
    group_size = HEADS // KV_HEADS
    places = jnp.arange(TOKENS, dtype=jnp.int32)
    turned_queries = rotary_turn(queries.astype(jnp.float32).reshape(TOKENS, HEADS, HEAD_DIM), places, 1.0).astype(jnp.bfloat16)
    turned_keys = rotary_turn(keys.astype(jnp.float32).reshape(TOKENS, KV_HEADS, HEAD_DIM), places, 1.0).astype(jnp.bfloat16)
    margin = ((WINDOW, WINDOW), (0, 0), (0, 0))
    padded_keys = jnp.pad(turned_keys, margin)
    padded_values = jnp.pad(values.reshape(TOKENS, KV_HEADS, HEAD_DIM), margin)
    sink_logit = sinks.astype(jnp.float32).reshape(KV_HEADS, group_size)[:, :, None, None]

    def one_block(block_index):
        start_row = block_index * WINDOW
        block_queries = lax.dynamic_slice_in_dim(turned_queries, start_row, WINDOW, 0).reshape(WINDOW, KV_HEADS, group_size, HEAD_DIM)
        block_keys = lax.dynamic_slice_in_dim(padded_keys, start_row, 3 * WINDOW, 0)
        block_values = lax.dynamic_slice_in_dim(padded_values, start_row, 3 * WINDOW, 0)
        scores = jnp.einsum('qkgd,mkd->kgqm', block_queries.astype(jnp.float32), block_keys.astype(jnp.float32)) * HEAD_DIM ** (-0.5)
        query_at = start_row + jnp.arange(WINDOW, dtype=jnp.int32)
        key_at = start_row - WINDOW + jnp.arange(3 * WINDOW, dtype=jnp.int32)
        allowed = (jnp.abs(query_at[:, None] - key_at[None, :]) <= WINDOW) & (key_at >= 0)[None, :] & (key_at < TOKENS)[None, :]
        scores = jnp.where(allowed[None, None], scores, NEG_LARGE)
        highest = jnp.maximum(lax.optimization_barrier(jnp.max(scores, axis=-1, keepdims=True)), sink_logit)
        lifted = jnp.exp(scores - highest)
        denominator = lax.optimization_barrier(jnp.sum(lifted, axis=-1, keepdims=True)) + jnp.exp(sink_logit - highest)
        probabilities = (lifted / denominator).astype(jnp.bfloat16)
        result = jnp.einsum('kgqm,mkd->qkgd', probabilities.astype(jnp.float32), block_values.astype(jnp.float32))
        return result.astype(jnp.bfloat16).reshape(WINDOW, HEADS * HEAD_DIM)
    blocks = lax.map(one_block, jnp.arange(TOKENS // WINDOW, dtype=jnp.int32))
    return blocks.reshape(TOKENS, HEADS * HEAD_DIM)

def gated_hidden(gathered_rows, gate_weight, up_weight):
    gate_values = jnp.dot(gathered_rows, gate_weight, preferred_element_type=jnp.float32)
    up_values = jnp.dot(gathered_rows, up_weight, preferred_element_type=jnp.float32)
    return (jax.nn.silu(gate_values) * up_values).astype(jnp.bfloat16)

def block_sum(hidden, down_weight):
    piece_width = hidden.shape[1] // N_TP
    running_total = jnp.zeros((hidden.shape[0], down_weight.shape[1]), jnp.float32)
    for block_index in range(N_TP):
        block_term = jnp.dot(hidden[:, block_index * piece_width:(block_index + 1) * piece_width], down_weight[block_index * piece_width:(block_index + 1) * piece_width], preferred_element_type=jnp.float32)
        running_total = running_total + lax.optimization_barrier(block_term.astype(jnp.bfloat16)).astype(jnp.float32)
    return running_total

def reference(queries, keys, values, sinks, residual, out_weight, norm_gain, shared_gate, shared_up, shared_down, expert_ids, route_weights, expert_gate, expert_up, expert_down):
    attended = attend(queries, keys, values, sinks)
    projected = jnp.dot(attended, out_weight, preferred_element_type=jnp.float32)
    mixed_rows = (residual.astype(jnp.float32) + projected).astype(jnp.bfloat16)
    mixed_float = mixed_rows.astype(jnp.float32)
    scale_rows = lax.rsqrt(lax.optimization_barrier(jnp.mean(mixed_float * mixed_float, axis=-1, keepdims=True)) + NORM_EPSILON)
    normed = (mixed_float * scale_rows * norm_gain).astype(jnp.bfloat16)
    shared_out = block_sum(gated_hidden(normed, shared_gate, shared_up), shared_down)
    owners = TOKENS // OWN
    assigns = OWN * TOPK
    route_rows = expert_ids.reshape(owners, assigns)
    order_index = jnp.arange(assigns, dtype=jnp.int32)
    earlier = order_index[None, :] < order_index[:, None]
    rank_in_block = lax.optimization_barrier(jnp.sum(((route_rows[:, :, None] == route_rows[:, None, :]) & earlier[None]).astype(jnp.int32), axis=2))
    slot_index = route_rows * CAP + rank_in_block
    owner_index = jnp.arange(owners, dtype=jnp.int32)[:, None]
    token_of = owner_index * OWN + order_index[None, :] // TOPK
    slot_token = jnp.full((owners, EXPERTS * CAP), TOKENS, jnp.int32).at[owner_index, slot_index].set(token_of)
    slot_weight = jnp.zeros((owners, EXPERTS * CAP), jnp.float32).at[owner_index, slot_index].set(route_weights.astype(jnp.float32).reshape(owners, assigns))
    normed_pad = jnp.concatenate([normed, jnp.zeros((1, D), jnp.bfloat16)], axis=0)

    def one_expert(accumulated, expert):
        tokens_here = lax.dynamic_slice_in_dim(slot_token, expert * CAP, CAP, 1).reshape(-1)
        weights_here = lax.dynamic_slice_in_dim(slot_weight, expert * CAP, CAP, 1).reshape(-1)
        gathered_rows = normed_pad[tokens_here]
        hidden = gated_hidden(gathered_rows, expert_gate[expert], expert_up[expert])
        outcome = block_sum(hidden, expert_down[expert]).astype(jnp.bfloat16)
        accumulated = accumulated.at[tokens_here].add(weights_here[:, None] * outcome.astype(jnp.float32))
        return (accumulated, None)
    accumulated, unused = lax.scan(one_expert, jnp.zeros((TOKENS + 1, D), jnp.float32), jnp.arange(EXPERTS, dtype=jnp.int32))
    return (mixed_float + shared_out + accumulated[:TOKENS]).astype(jnp.bfloat16)
```

```python
import jax
import jax.numpy as jnp
from jax import lax
from jax.experimental import pallas as pl
from jax.experimental.pallas import tpu as pltpu
from jax.sharding import PartitionSpec as P
import functools

MESH = pl.DeviceIdType.MESH
VMEM = pl.BlockSpec(memory_space=pltpu.VMEM)
VMEM_LIMIT = 60 * 1024 * 1024

HEAD_DIM = 64
WINDOW = 128
GRID_W = 64
TOPK = 2


ROPE_BASE = 10000.0
NEG_LARGE = -1e30
NORM_EPSILON = 1e-06


def extended(x, sides, width):
    for axis, dim in sides:
        size, length = (lax.axis_size(axis), x.shape[dim])
        up = [(i, (i + 1) % size) for i in range(size - 1)]
        down = [(j, i) for i, j in up]
        last = lax.slice_in_dim(x, length - width, length, axis=dim)
        initial = lax.slice_in_dim(x, 0, width, axis=dim)
        before = lax.ppermute(last, axis, up)
        after = lax.ppermute(initial, axis, down)
        x = jnp.concatenate([before, x, after], axis=dim)
    return x


def rotary_turn(values, places, turn_sign):
    halfway = values.shape[-1] // 2
    quarter = halfway // 2
    spectrum = ROPE_BASE ** (-jnp.arange(0, halfway, 2, dtype=jnp.float32) / halfway)

    def rotate_by(segment, offsets_at):
        angles = turn_sign * offsets_at.astype(jnp.float32)[:, None] * spectrum[None, :]
        cosine = jnp.cos(angles)[:, None, :]
        sine_part = jnp.sin(angles)[:, None, :]
        former = segment[..., :quarter]
        latter = segment[..., quarter:]
        return jnp.concatenate(
            [former * cosine - latter * sine_part, former * sine_part + latter * cosine], axis=-1
        )

    return jnp.concatenate(
        [
            rotate_by(values[..., :halfway], places // GRID_W),
            rotate_by(values[..., halfway:], places % GRID_W),
        ],
        axis=-1,
    )


def gated_hidden(gathered_rows, gate_weight, up_weight):
    gate_values = jnp.dot(gathered_rows, gate_weight, preferred_element_type=jnp.float32)
    up_values = jnp.dot(gathered_rows, up_weight, preferred_element_type=jnp.float32)
    return (jax.nn.silu(gate_values) * up_values).astype(jnp.bfloat16)


def places_of(token_split, width_split):
    sp_at = lax.axis_index("sp")
    tp_at = lax.axis_index("tp")
    pair = tp_at + 1 - 2 * (tp_at % 2)
    cross = (tp_at + width_split // 2) % width_split
    return sp_at, tp_at, pair, cross


def greet(token_split, sp_at, tp_at, pair, cross):
    barrier = pltpu.get_barrier_semaphore()

    @pl.loop(1, token_split)
    def _(i):
        pl.semaphore_signal(
            barrier, inc=1, device_id=((sp_at + i) % token_split, tp_at), device_id_type=MESH
        )

    for partner in (pair, cross):
        pl.semaphore_signal(barrier, inc=1, device_id=(sp_at, partner), device_id_type=MESH)
    pl.semaphore_wait(barrier, token_split + 1)


def dispatch_kernel(token_split, width_split, rows_ref, out_ref, local_sem, send, recv):
    sp_at, tp_at, pair, cross = places_of(token_split, width_split)
    greet(token_split, sp_at, tp_at, pair, cross)

    def remote(stage, i, source, target, where):
        return pltpu.make_async_remote_copy(
            src_ref=source,
            dst_ref=target,
            send_sem=send.at[stage, i],
            recv_sem=recv.at[stage, i],
            device_id=where,
            device_id_type=MESH,
        )

    def along(i):
        there = (sp_at + i) % token_split
        return remote(0, i, rows_ref.at[there], out_ref.at[:, tp_at, sp_at], (there, tp_at))

    def passed(stage, i, block, partner):
        piece = out_ref.at[:, block, (sp_at + token_split - i) % token_split]
        return remote(stage, i, piece, piece, (sp_at, partner))

    @pl.loop(1, token_split)
    def _(i):
        along(i).start()

    own = pltpu.make_async_copy(rows_ref.at[sp_at], out_ref.at[:, tp_at, sp_at], local_sem)
    own.start()
    own.wait()
    passed(1, 0, tp_at, cross).start()
    passed(2, 0, tp_at, pair).start()

    @pl.loop(1, token_split)
    def _(i):
        along(i).wait_recv()
        passed(1, i, tp_at, cross).start()
        passed(2, i, tp_at, pair).start()

    @pl.loop(0, token_split)
    def _(i):
        passed(1, i, tp_at, cross).wait_recv()
        passed(3, i, cross, pair).start()

    @pl.loop(0, token_split)
    def _(i):
        passed(2, i, tp_at, pair).wait()
        passed(1, i, tp_at, cross).wait_send()
        passed(3, i, cross, pair).wait()

    @pl.loop(1, token_split)
    def _(i):
        along(i).wait_send()


def dispatch(rows, token_split, width_split):
    _, experts, cap, width = rows.shape
    return pl.pallas_call(
        functools.partial(dispatch_kernel, token_split, width_split),
        out_shape=jax.ShapeDtypeStruct(
            (experts, width_split, token_split, cap, width), rows.dtype
        ),
        in_specs=[VMEM],
        out_specs=VMEM,
        scratch_shapes=[
            pltpu.SemaphoreType.DMA,
            pltpu.SemaphoreType.DMA((4, token_split)),
            pltpu.SemaphoreType.DMA((4, token_split)),
        ],
        compiler_params=pltpu.CompilerParams(
            collective_id=1, has_side_effects=True, vmem_limit_bytes=VMEM_LIMIT
        ),
        name="dispatch",
    )(rows)


def collect_kernel(
    token_split,
    width_split,
    part_ref,
    shared_ref,
    back_ref,
    shared_out,
    from_pair,
    to_cross,
    from_cross,
    final,
    shared_pair,
    shared_cross,
    shared_got,
    send,
    recv,
    shared_send,
    shared_recv,
):
    sp_at, tp_at, pair, cross = places_of(token_split, width_split)
    pair_cross = (pair + width_split // 2) % width_split
    greet(token_split, sp_at, tp_at, pair, cross)

    def copy(source, target, sems, where):
        return pltpu.make_async_remote_copy(
            src_ref=source,
            dst_ref=target,
            send_sem=sems[0],
            recv_sem=sems[1],
            device_id=where,
            device_id_type=MESH,
        )

    def at(stage, i):
        return send.at[stage, i], recv.at[stage, i]

    def at_shared(stage):
        return shared_send.at[stage], shared_recv.at[stage]

    def place(i):
        return (sp_at + 1 + i) % token_split

    def pair_copy(side, i):
        block = pair_cross if side == 0 else pair
        there = place(i)
        return copy(
            part_ref.at[:, block, there], from_pair.at[side, there], at(side, i), (sp_at, pair)
        )

    def cross_copy(i):
        there = place(i)
        return copy(to_cross.at[there], from_cross.at[there], at(2, i), (sp_at, cross))

    def along_copy(i):
        there = place(i)
        return copy(final.at[there], back_ref.at[sp_at], at(3, i), (there, tp_at))

    def shared_copy(side):
        block = pair_cross if side == 0 else pair
        return copy(shared_ref.at[block], shared_pair.at[side], at_shared(side), (sp_at, pair))

    shared_over = copy(shared_cross, shared_got, at_shared(2), (sp_at, cross))

    @pl.loop(0, token_split)
    def _(i):
        pair_copy(0, i).start()

    shared_copy(0).start()

    @pl.loop(0, token_split)
    def _(i):
        pair_copy(1, i).start()

    shared_copy(1).start()

    def total(*terms):
        value = terms[0].astype(jnp.float32)
        for term in terms[1:]:
            value = value + term.astype(jnp.float32)
        return value

    @pl.loop(0, token_split)
    def _(i):
        there = place(i)
        pair_copy(0, i).wait_recv()
        to_cross[there] = total(part_ref[:, cross, there], from_pair[0, there]).astype(
            to_cross.dtype
        )
        cross_copy(i).start()

    shared_copy(0).wait_recv()
    shared_cross[...] = total(shared_ref[cross], shared_pair[0]).astype(shared_cross.dtype)
    shared_over.start()

    def summed(i):
        there = place(i)
        pair_copy(1, i).wait_recv()
        cross_copy(i).wait_recv()
        return total(part_ref[:, tp_at, there], from_pair[1, there], from_cross[there]).astype(
            back_ref.dtype
        )

    @pl.loop(0, token_split - 1)
    def _(i):
        final[place(i)] = summed(i)
        along_copy(i).start()

    back_ref[sp_at] = summed(token_split - 1)
    shared_copy(1).wait_recv()
    shared_over.wait_recv()
    shared_out[...] = total(shared_ref[tp_at], shared_pair[1], shared_got[...])

    @pl.loop(0, token_split)
    def _(i):
        pair_copy(0, i).wait_send()
        pair_copy(1, i).wait_send()
        cross_copy(i).wait_send()

    shared_copy(0).wait_send()
    shared_copy(1).wait_send()
    shared_over.wait_send()

    @pl.loop(0, token_split - 1)
    def _(i):
        along_copy(i).wait()


def collect(part, shared, token_split, width_split):
    experts, _, _, cap, width = part.shape
    own = shared.shape[1]
    block = (token_split, experts, cap, width)
    kind = part.dtype
    return pl.pallas_call(
        functools.partial(collect_kernel, token_split, width_split),
        out_shape=(
            jax.ShapeDtypeStruct(block, kind),
            jax.ShapeDtypeStruct((own, width), jnp.float32),
        ),
        in_specs=[VMEM] * 2,
        out_specs=(VMEM, VMEM),
        scratch_shapes=[
            pltpu.VMEM((2,) + block, kind),
            pltpu.VMEM(block, kind),
            pltpu.VMEM(block, kind),
            pltpu.VMEM(block, kind),
            pltpu.VMEM((2, own, width), kind),
            pltpu.VMEM((own, width), kind),
            pltpu.VMEM((own, width), kind),
            pltpu.SemaphoreType.DMA((4, token_split)),
            pltpu.SemaphoreType.DMA((4, token_split)),
            pltpu.SemaphoreType.DMA((3,)),
            pltpu.SemaphoreType.DMA((3,)),
        ],
        compiler_params=pltpu.CompilerParams(
            collective_id=2, has_side_effects=True, vmem_limit_bytes=VMEM_LIMIT
        ),
        name="collect",
    )(part, shared)


def per_device(
    queries,
    keys,
    values,
    sinks,
    residual,
    out_weight,
    norm_gain,
    shared_gate,
    shared_up,
    shared_down,
    expert_ids,
    route_weights,
    expert_gate,
    expert_up,
    expert_down,
):
    block_rows = queries.shape[0]
    width_split = lax.axis_size("tp")
    token_split = lax.axis_size("sp")
    width_index = lax.axis_index("tp")
    key_heads = keys.shape[1] // HEAD_DIM
    heads_local = queries.shape[1] // HEAD_DIM
    group_size = heads_local // key_heads
    first_row = lax.axis_index("sp") * block_rows
    total_rows = token_split * block_rows
    places = first_row + jnp.arange(block_rows, dtype=jnp.int32)
    turned_queries = rotary_turn(
        queries.astype(jnp.float32).reshape(block_rows, heads_local, HEAD_DIM), places, 1.0
    ).astype(jnp.bfloat16)
    turned_keys = rotary_turn(
        keys.astype(jnp.float32).reshape(block_rows, key_heads, HEAD_DIM), places, 1.0
    ).astype(jnp.bfloat16)
    joined = jnp.concatenate(
        [turned_keys.reshape(block_rows, key_heads * HEAD_DIM), values], axis=1
    )
    widened = extended(joined, (("sp", 0),), WINDOW)
    blocks = block_rows // WINDOW
    windows = jnp.concatenate(
        [
            widened[shift_index * WINDOW : shift_index * WINDOW + blocks * WINDOW].reshape(
                blocks, WINDOW, -1
            )
            for shift_index in range(3)
        ],
        axis=1,
    )
    key_win = windows[..., : key_heads * HEAD_DIM].reshape(blocks, 3 * WINDOW, key_heads, HEAD_DIM)
    value_win = windows[..., key_heads * HEAD_DIM :].reshape(
        blocks, 3 * WINDOW, key_heads, HEAD_DIM
    )
    query_blocks = turned_queries.reshape(blocks, WINDOW, key_heads, group_size, HEAD_DIM)
    scores = jnp.einsum(
        "bqkgd,bmkd->bkgqm", query_blocks, key_win, preferred_element_type=jnp.float32
    ) * HEAD_DIM ** (-0.5)
    block_first = first_row + jnp.arange(blocks, dtype=jnp.int32) * WINDOW
    query_at = block_first[:, None, None] + jnp.arange(WINDOW, dtype=jnp.int32)[None, :, None]
    key_at = (
        block_first[:, None, None] - WINDOW + jnp.arange(3 * WINDOW, dtype=jnp.int32)[None, None, :]
    )
    allowed = (jnp.abs(query_at - key_at) <= WINDOW) & (key_at >= 0) & (key_at < total_rows)
    scores = jnp.where(allowed[:, None, None], scores, NEG_LARGE)
    sink_logit = sinks.reshape(key_heads, group_size)[None, :, :, None, None]
    highest = jnp.maximum(jnp.max(scores, axis=-1, keepdims=True), sink_logit)
    lifted = jnp.exp(scores - highest)
    denominator = jnp.sum(lifted, axis=-1, keepdims=True) + jnp.exp(sink_logit - highest)
    probabilities = (lifted / denominator).astype(jnp.bfloat16)
    attended = jnp.einsum(
        "bkgqm,bmkd->bqkgd", probabilities, value_win, preferred_element_type=jnp.float32
    )
    attended = attended.astype(jnp.bfloat16).reshape(block_rows, heads_local * HEAD_DIM)
    model_width = out_weight.shape[1]
    projected = jnp.dot(
        lax.all_gather(attended, "tp", axis=1, tiled=True),
        out_weight,
        preferred_element_type=jnp.float32,
    )
    mixed_rows = (residual.astype(jnp.float32) + projected).astype(jnp.bfloat16)
    mixed_float = mixed_rows.astype(jnp.float32)
    scale_rows = lax.rsqrt(
        jnp.mean(mixed_float * mixed_float, axis=-1, keepdims=True) + NORM_EPSILON
    )
    normed = (mixed_float * scale_rows * norm_gain).astype(jnp.bfloat16)
    own_rows = block_rows // width_split
    shared_hidden = gated_hidden(normed, shared_gate, shared_up)
    shared_part = jnp.dot(shared_hidden, shared_down, preferred_element_type=jnp.float32)
    shared_part = shared_part.astype(jnp.bfloat16).reshape(width_split, own_rows, model_width)
    experts_here = expert_gate.shape[0]
    experts_all = experts_here * token_split
    capacity = max(2, 2 * own_rows * TOPK // experts_all)
    own_start = width_index * own_rows
    own_ids = lax.dynamic_slice_in_dim(expert_ids, own_start, own_rows, 0)
    own_routes = own_ids.reshape(own_rows * TOPK)
    order_index = jnp.arange(own_rows * TOPK, dtype=jnp.int32)
    matches = (own_routes[:, None] == own_routes[None, :]) & (
        order_index[None, :] < order_index[:, None]
    )
    rank_in_block = jnp.sum(matches.astype(jnp.int32), axis=1)
    slots = (own_routes * capacity + rank_in_block).reshape(own_rows, TOPK)
    slot_count = experts_all * capacity
    chosen = slots[:, :, None] == jnp.arange(slot_count, dtype=jnp.int32)[None, None, :]
    sender = jnp.any(chosen, axis=1).astype(jnp.bfloat16)
    normed_own = lax.dynamic_slice_in_dim(normed, own_start, own_rows, 0)
    outgoing = lax.dot_general(
        sender, normed_own, (((0,), (0,)), ((), ())), preferred_element_type=jnp.float32
    ).astype(jnp.bfloat16)
    outgoing = outgoing.reshape(token_split, experts_here, capacity, model_width)
    arrived = dispatch(outgoing, token_split, width_split)
    slot_batch = arrived.reshape(experts_here, -1, model_width)
    gate_values = jnp.einsum(
        "erd,edh->erh", slot_batch, expert_gate, preferred_element_type=jnp.float32
    )
    up_values = jnp.einsum(
        "erd,edh->erh", slot_batch, expert_up, preferred_element_type=jnp.float32
    )
    hidden = (jax.nn.silu(gate_values) * up_values).astype(jnp.bfloat16)
    partial_value = jnp.einsum(
        "erh,ehd->erd", hidden, expert_down, preferred_element_type=jnp.float32
    ).astype(jnp.bfloat16)
    returned, shared_sum = collect(
        partial_value.reshape(arrived.shape), shared_part, token_split, width_split
    )
    flat_back = returned.reshape(slot_count, model_width)
    weights = jnp.sum(jnp.where(chosen, route_weights[:, :, None], 0.0), axis=1)
    coarse = weights.astype(jnp.bfloat16)
    fine = (weights - coarse.astype(jnp.float32)).astype(jnp.bfloat16)
    routed = jnp.dot(
        jnp.concatenate([coarse, fine], axis=0), flat_back, preferred_element_type=jnp.float32
    )
    routed = routed[:own_rows] + routed[own_rows:]
    mixed_own = lax.dynamic_slice_in_dim(mixed_float, own_start, own_rows, 0)
    return (mixed_own + shared_sum + routed).astype(jnp.bfloat16)


def solution(mesh):
    placed = (
        P("sp", "tp"),
        P("sp", "tp"),
        P("sp", "tp"),
        P("tp"),
        P("sp", None),
        P(),
        P(),
        P(None, "tp"),
        P(None, "tp"),
        P("tp", None),
        P("sp", None),
        P(("sp", "tp"), None),
        P("sp", None, "tp"),
        P("sp", None, "tp"),
        P("sp", "tp", None),
    )
    return jax.shard_map(
        per_device, mesh=mesh, in_specs=placed, out_specs=P(("sp", "tp"), None), check_vma=False
    )
```

```python
import jax
import jax.numpy as jnp
import numpy as np
from jax import lax
from jax.experimental import pallas as pl
from jax.experimental.pallas import tpu as pltpu
from jax.sharding import PartitionSpec as P
import functools

MESH = pl.DeviceIdType.MESH
VMEM = pl.BlockSpec(memory_space=pltpu.VMEM)
VMEM_LIMIT = 60 * 1024 * 1024

HEAD_DIM = 64
WINDOW = 128
GRID_W = 64
TOPK = 2


ROPE_BASE = 10000.0
NEG_LARGE = -1e30
NORM_EPSILON = 1e-06


def extended(x, sides, width):
    for axis, dim in sides:
        size, length = (lax.axis_size(axis), x.shape[dim])
        up = [(i, (i + 1) % size) for i in range(size - 1)]
        down = [(j, i) for i, j in up]
        last = lax.slice_in_dim(x, length - width, length, axis=dim)
        initial = lax.slice_in_dim(x, 0, width, axis=dim)
        before = lax.ppermute(last, axis, up)
        after = lax.ppermute(initial, axis, down)
        x = jnp.concatenate([before, x, after], axis=dim)
    return x


def rotary_turn(values, places):
    heads = values.shape[1] // HEAD_DIM
    halfway = HEAD_DIM // 2
    quarter = halfway // 2
    column = np.arange(HEAD_DIM)
    swap = np.zeros((HEAD_DIM, HEAD_DIM), np.float32)
    for d in range(HEAD_DIM):
        if d % halfway < quarter:
            swap[d + quarter, d] = -1.0
        else:
            swap[d - quarter, d] = 1.0
    swap = jnp.asarray(np.kron(np.eye(heads, dtype=np.float32), swap), jnp.bfloat16)
    spectrum = ROPE_BASE ** (-jnp.arange(0, halfway, 2, dtype=jnp.float32) / halfway)
    spectrum = jnp.tile(spectrum, values.shape[1] // quarter)
    first_half = jnp.asarray(np.tile(column < halfway, heads))
    offsets = jnp.where(
        first_half[None, :], (places // GRID_W)[:, None], (places % GRID_W)[:, None]
    )
    angles = offsets.astype(jnp.float32) * spectrum[None, :]
    swapped = jnp.dot(values, swap, preferred_element_type=jnp.float32)
    return (values.astype(jnp.float32) * jnp.cos(angles) + swapped * jnp.sin(angles)).astype(
        jnp.bfloat16
    )


def attend_kernel(key_heads, total_rows, first_ref, sink_ref, q_ref, kv_ref, out_ref):
    first = first_ref[0]
    heads = q_ref.shape[1] // HEAD_DIM
    group = heads // key_heads
    shape = (WINDOW, 3 * WINDOW)
    row = lax.broadcasted_iota(jnp.int32, shape, 0)
    column = lax.broadcasted_iota(jnp.int32, shape, 1) - WINDOW
    near = jnp.abs(row - column) <= WINDOW
    for block in range(q_ref.shape[0] // WINDOW):
        start = block * WINDOW
        key_at = column + (first + start)
        allowed = near & (key_at >= 0) & (key_at < total_rows)
        for kh in range(key_heads):
            span = slice(start, start + 3 * WINDOW)
            key = kv_ref[span, kh * HEAD_DIM : (kh + 1) * HEAD_DIM]
            value = kv_ref[span, (key_heads + kh) * HEAD_DIM : (key_heads + kh + 1) * HEAD_DIM]
            for h in range(kh * group, (kh + 1) * group):
                query = q_ref[start : start + WINDOW, h * HEAD_DIM : (h + 1) * HEAD_DIM]
                scores = lax.dot_general(
                    query, key, (((1,), (1,)), ((), ())), preferred_element_type=jnp.float32
                ) * HEAD_DIM ** (-0.5)
                scores = jnp.where(allowed, scores, NEG_LARGE)
                sink = sink_ref[h]
                highest = jnp.maximum(jnp.max(scores, axis=1, keepdims=True), sink)
                lifted = jnp.exp(scores - highest)
                below = jnp.sum(lifted, axis=1, keepdims=True) + jnp.exp(sink - highest)
                chances = (lifted / below).astype(jnp.bfloat16)
                result = jnp.dot(chances, value, preferred_element_type=jnp.float32)
                out_ref[start : start + WINDOW, h * HEAD_DIM : (h + 1) * HEAD_DIM] = result.astype(
                    jnp.bfloat16
                )


def attend(first, sinks, turned, widened, key_heads, total_rows):
    smem = pl.BlockSpec(memory_space=pltpu.SMEM)
    return pl.pallas_call(
        functools.partial(attend_kernel, key_heads, total_rows),
        out_shape=jax.ShapeDtypeStruct(turned.shape, jnp.bfloat16),
        in_specs=[smem, smem, VMEM, VMEM],
        out_specs=VMEM,
        name="attend",
    )(first.reshape(1), sinks, turned, widened)


def routes_kernel(capacity, ids_ref, ids_row_ref, weights_ref, sender_ref, weigh_ref):
    own, slot_count = sender_ref.shape
    earlier = lax.broadcasted_iota(jnp.int32, (own, own), 1) < lax.broadcasted_iota(
        jnp.int32, (own, own), 0
    )
    slot_of = lax.broadcasted_iota(jnp.int32, (own, slot_count), 1)
    taken = jnp.zeros((own, slot_count), jnp.float32)
    weigh = jnp.zeros((own, slot_count), jnp.float32)
    for k in range(TOPK):
        mine = ids_ref[:, k : k + 1]
        rank = jnp.zeros((own, 1), jnp.int32)
        for other in range(TOPK):
            same = (ids_row_ref[other : other + 1, :] == mine) & earlier
            rank = rank + jnp.sum(same.astype(jnp.int32), axis=1, keepdims=True)
        chosen = slot_of == mine * capacity + rank
        taken = jnp.where(chosen, 1.0, taken)
        weigh = jnp.where(chosen, weights_ref[:, k : k + 1], weigh)
    sender_ref[...] = taken.astype(jnp.bfloat16)
    coarse = weigh.astype(jnp.bfloat16)
    weigh_ref[:own, :] = coarse
    weigh_ref[own:, :] = (weigh - coarse.astype(jnp.float32)).astype(jnp.bfloat16)


def routes(own_ids, weights, capacity, slot_count):
    own = own_ids.shape[0]
    return pl.pallas_call(
        functools.partial(routes_kernel, capacity),
        out_shape=(
            jax.ShapeDtypeStruct((own, slot_count), jnp.bfloat16),
            jax.ShapeDtypeStruct((2 * own, slot_count), jnp.bfloat16),
        ),
        in_specs=[VMEM] * 3,
        out_specs=(VMEM, VMEM),
        name="routes",
    )(own_ids, own_ids.T, weights)


def gated_hidden(gathered_rows, gate_weight, up_weight):
    gate_values = jnp.dot(gathered_rows, gate_weight, preferred_element_type=jnp.float32)
    up_values = jnp.dot(gathered_rows, up_weight, preferred_element_type=jnp.float32)
    return (jax.nn.silu(gate_values) * up_values).astype(jnp.bfloat16)


def places_of(token_split, width_split):
    sp_at = lax.axis_index("sp")
    tp_at = lax.axis_index("tp")
    pair = tp_at + 1 - 2 * (tp_at % 2)
    cross = (tp_at + width_split // 2) % width_split
    return sp_at, tp_at, pair, cross


def greet(token_split, sp_at, tp_at, pair, cross):
    barrier = pltpu.get_barrier_semaphore()

    @pl.loop(1, token_split)
    def _(i):
        pl.semaphore_signal(
            barrier, inc=1, device_id=((sp_at + i) % token_split, tp_at), device_id_type=MESH
        )

    for partner in (pair, cross):
        pl.semaphore_signal(barrier, inc=1, device_id=(sp_at, partner), device_id_type=MESH)
    pl.semaphore_wait(barrier, token_split + 1)


def dispatch_kernel(
    token_split,
    width_split,
    rows_ref,
    normed_ref,
    gate_ref,
    up_ref,
    down_ref,
    out_ref,
    shared_ref,
    local_sem,
    send,
    recv,
):
    sp_at, tp_at, pair, cross = places_of(token_split, width_split)
    greet(token_split, sp_at, tp_at, pair, cross)

    def remote(stage, i, source, target, where):
        return pltpu.make_async_remote_copy(
            src_ref=source,
            dst_ref=target,
            send_sem=send.at[stage, i],
            recv_sem=recv.at[stage, i],
            device_id=where,
            device_id_type=MESH,
        )

    def along(i):
        there = (sp_at + i) % token_split
        return remote(0, i, rows_ref.at[there], out_ref.at[:, tp_at, sp_at], (there, tp_at))

    def passed(stage, i, block, partner):
        piece = out_ref.at[:, block, (sp_at + token_split - i) % token_split]
        return remote(stage, i, piece, piece, (sp_at, partner))

    @pl.loop(1, token_split)
    def _(i):
        along(i).start()

    own = pltpu.make_async_copy(rows_ref.at[sp_at], out_ref.at[:, tp_at, sp_at], local_sem)
    own.start()
    own.wait()
    passed(1, 0, tp_at, cross).start()
    passed(2, 0, tp_at, pair).start()

    @pl.loop(1, token_split)
    def _(i):
        along(i).wait_recv()
        passed(1, i, tp_at, cross).start()
        passed(2, i, tp_at, pair).start()

    own_rows = shared_ref.shape[1]
    for block in range(width_split):
        here = normed_ref[block * own_rows : (block + 1) * own_rows, :]
        hidden = gated_hidden(here, gate_ref[...], up_ref[...])
        shared_ref[block] = jnp.dot(
            hidden, down_ref[...], preferred_element_type=jnp.float32
        ).astype(shared_ref.dtype)

    @pl.loop(0, token_split)
    def _(i):
        passed(1, i, tp_at, cross).wait_recv()
        passed(3, i, cross, pair).start()

    @pl.loop(0, token_split)
    def _(i):
        passed(2, i, tp_at, pair).wait()
        passed(1, i, tp_at, cross).wait_send()
        passed(3, i, cross, pair).wait()

    @pl.loop(1, token_split)
    def _(i):
        along(i).wait_send()


def dispatch(rows, normed, gate, up, down, token_split, width_split):
    _, experts, cap, width = rows.shape
    return pl.pallas_call(
        functools.partial(dispatch_kernel, token_split, width_split),
        out_shape=(
            jax.ShapeDtypeStruct((experts, width_split, token_split, cap, width), rows.dtype),
            jax.ShapeDtypeStruct(
                (width_split, normed.shape[0] // width_split, width), rows.dtype
            ),
        ),
        in_specs=[VMEM] * 5,
        out_specs=(VMEM, VMEM),
        scratch_shapes=[
            pltpu.SemaphoreType.DMA,
            pltpu.SemaphoreType.DMA((4, token_split)),
            pltpu.SemaphoreType.DMA((4, token_split)),
        ],
        compiler_params=pltpu.CompilerParams(
            collective_id=1, has_side_effects=True, vmem_limit_bytes=VMEM_LIMIT
        ),
        name="dispatch",
    )(rows, normed, gate, up, down)


def collect_kernel(
    token_split,
    width_split,
    part_ref,
    shared_ref,
    back_ref,
    shared_out,
    from_pair,
    to_cross,
    from_cross,
    final,
    shared_pair,
    shared_cross,
    shared_got,
    send,
    recv,
    shared_send,
    shared_recv,
):
    sp_at, tp_at, pair, cross = places_of(token_split, width_split)
    pair_cross = (pair + width_split // 2) % width_split
    greet(token_split, sp_at, tp_at, pair, cross)

    def copy(source, target, sems, where):
        return pltpu.make_async_remote_copy(
            src_ref=source,
            dst_ref=target,
            send_sem=sems[0],
            recv_sem=sems[1],
            device_id=where,
            device_id_type=MESH,
        )

    def at(stage, i):
        return send.at[stage, i], recv.at[stage, i]

    def at_shared(stage):
        return shared_send.at[stage], shared_recv.at[stage]

    def place(i):
        return (sp_at + 1 + i) % token_split

    def pair_copy(side, i):
        block = pair_cross if side == 0 else pair
        there = place(i)
        return copy(
            part_ref.at[:, block, there], from_pair.at[side, there], at(side, i), (sp_at, pair)
        )

    def cross_copy(i):
        there = place(i)
        return copy(to_cross.at[there], from_cross.at[there], at(2, i), (sp_at, cross))

    def along_copy(i):
        there = place(i)
        return copy(final.at[there], back_ref.at[sp_at], at(3, i), (there, tp_at))

    def shared_copy(side):
        block = pair_cross if side == 0 else pair
        return copy(shared_ref.at[block], shared_pair.at[side], at_shared(side), (sp_at, pair))

    shared_over = copy(shared_cross, shared_got, at_shared(2), (sp_at, cross))

    @pl.loop(0, token_split)
    def _(i):
        pair_copy(0, i).start()

    shared_copy(0).start()

    @pl.loop(0, token_split)
    def _(i):
        pair_copy(1, i).start()

    shared_copy(1).start()

    def total(*terms):
        value = terms[0].astype(jnp.float32)
        for term in terms[1:]:
            value = value + term.astype(jnp.float32)
        return value

    @pl.loop(0, token_split)
    def _(i):
        there = place(i)
        pair_copy(0, i).wait_recv()
        to_cross[there] = total(part_ref[:, cross, there], from_pair[0, there]).astype(
            to_cross.dtype
        )
        cross_copy(i).start()

    shared_copy(0).wait_recv()
    shared_cross[...] = total(shared_ref[cross], shared_pair[0]).astype(shared_cross.dtype)
    shared_over.start()

    def summed(i):
        there = place(i)
        pair_copy(1, i).wait_recv()
        cross_copy(i).wait_recv()
        return total(part_ref[:, tp_at, there], from_pair[1, there], from_cross[there]).astype(
            back_ref.dtype
        )

    @pl.loop(0, token_split - 1)
    def _(i):
        final[place(i)] = summed(i)
        along_copy(i).start()

    back_ref[sp_at] = summed(token_split - 1)
    shared_copy(1).wait_recv()
    shared_over.wait_recv()
    shared_out[...] = total(shared_ref[tp_at], shared_pair[1], shared_got[...])

    @pl.loop(0, token_split)
    def _(i):
        pair_copy(0, i).wait_send()
        pair_copy(1, i).wait_send()
        cross_copy(i).wait_send()

    shared_copy(0).wait_send()
    shared_copy(1).wait_send()
    shared_over.wait_send()

    @pl.loop(0, token_split - 1)
    def _(i):
        along_copy(i).wait()


def collect(part, shared, token_split, width_split):
    experts, _, _, cap, width = part.shape
    own = shared.shape[1]
    block = (token_split, experts, cap, width)
    kind = part.dtype
    return pl.pallas_call(
        functools.partial(collect_kernel, token_split, width_split),
        out_shape=(
            jax.ShapeDtypeStruct(block, kind),
            jax.ShapeDtypeStruct((own, width), jnp.float32),
        ),
        in_specs=[VMEM] * 2,
        out_specs=(VMEM, VMEM),
        scratch_shapes=[
            pltpu.VMEM((2,) + block, kind),
            pltpu.VMEM(block, kind),
            pltpu.VMEM(block, kind),
            pltpu.VMEM(block, kind),
            pltpu.VMEM((2, own, width), kind),
            pltpu.VMEM((own, width), kind),
            pltpu.VMEM((own, width), kind),
            pltpu.SemaphoreType.DMA((4, token_split)),
            pltpu.SemaphoreType.DMA((4, token_split)),
            pltpu.SemaphoreType.DMA((3,)),
            pltpu.SemaphoreType.DMA((3,)),
        ],
        compiler_params=pltpu.CompilerParams(
            collective_id=2, has_side_effects=True, vmem_limit_bytes=VMEM_LIMIT
        ),
        name="collect",
    )(part, shared)


def per_device(
    queries,
    keys,
    values,
    sinks,
    residual,
    out_weight,
    norm_gain,
    shared_gate,
    shared_up,
    shared_down,
    expert_ids,
    route_weights,
    expert_gate,
    expert_up,
    expert_down,
):
    block_rows = queries.shape[0]
    width_split = lax.axis_size("tp")
    token_split = lax.axis_size("sp")
    width_index = lax.axis_index("tp")
    key_heads = keys.shape[1] // HEAD_DIM
    heads_local = queries.shape[1] // HEAD_DIM
    first_row = lax.axis_index("sp") * block_rows
    total_rows = token_split * block_rows
    places = first_row + jnp.arange(block_rows, dtype=jnp.int32)
    turned = rotary_turn(jnp.concatenate([queries, keys], axis=1), places)
    query_width = heads_local * HEAD_DIM
    joined = jnp.concatenate([turned[:, query_width:], values], axis=1)
    widened = extended(joined, (("sp", 0),), WINDOW)
    attended = attend(
        first_row, sinks, turned[:, :query_width], widened, key_heads, total_rows
    )
    model_width = out_weight.shape[1]
    projected = jnp.dot(
        lax.all_gather(attended, "tp", axis=1, tiled=True),
        out_weight,
        preferred_element_type=jnp.float32,
    )
    mixed_rows = (residual.astype(jnp.float32) + projected).astype(jnp.bfloat16)
    mixed_float = mixed_rows.astype(jnp.float32)
    scale_rows = lax.rsqrt(
        jnp.mean(mixed_float * mixed_float, axis=-1, keepdims=True) + NORM_EPSILON
    )
    normed = (mixed_float * scale_rows * norm_gain).astype(jnp.bfloat16)
    own_rows = block_rows // width_split
    experts_here = expert_gate.shape[0]
    experts_all = experts_here * token_split
    capacity = max(2, 2 * own_rows * TOPK // experts_all)
    own_start = width_index * own_rows
    own_ids = lax.dynamic_slice_in_dim(expert_ids, own_start, own_rows, 0)
    slot_count = experts_all * capacity
    sender, weigh = routes(own_ids, route_weights, capacity, slot_count)
    normed_own = lax.dynamic_slice_in_dim(normed, own_start, own_rows, 0)
    outgoing = lax.dot_general(
        sender, normed_own, (((0,), (0,)), ((), ())), preferred_element_type=jnp.float32
    ).astype(jnp.bfloat16)
    outgoing = outgoing.reshape(token_split, experts_here, capacity, model_width)
    arrived, shared_part = dispatch(
        outgoing, normed, shared_gate, shared_up, shared_down, token_split, width_split
    )
    slot_batch = arrived.reshape(experts_here, -1, model_width)
    gate_values = jnp.einsum(
        "erd,edh->erh", slot_batch, expert_gate, preferred_element_type=jnp.float32
    )
    up_values = jnp.einsum(
        "erd,edh->erh", slot_batch, expert_up, preferred_element_type=jnp.float32
    )
    hidden = (jax.nn.silu(gate_values) * up_values).astype(jnp.bfloat16)
    partial_value = jnp.einsum(
        "erh,ehd->erd", hidden, expert_down, preferred_element_type=jnp.float32
    ).astype(jnp.bfloat16)
    returned, shared_sum = collect(
        partial_value.reshape(arrived.shape), shared_part, token_split, width_split
    )
    flat_back = returned.reshape(slot_count, model_width)
    routed = jnp.dot(weigh, flat_back, preferred_element_type=jnp.float32)
    routed = routed[:own_rows] + routed[own_rows:]
    mixed_own = lax.dynamic_slice_in_dim(mixed_float, own_start, own_rows, 0)
    return (mixed_own + shared_sum + routed).astype(jnp.bfloat16)


def solution(mesh):
    placed = (
        P("sp", "tp"),
        P("sp", "tp"),
        P("sp", "tp"),
        P("tp"),
        P("sp", None),
        P(),
        P(),
        P(None, "tp"),
        P(None, "tp"),
        P("tp", None),
        P("sp", None),
        P(("sp", "tp"), None),
        P("sp", None, "tp"),
        P("sp", None, "tp"),
        P("sp", "tp", None),
    )
    return jax.shard_map(
        per_device, mesh=mesh, in_specs=placed, out_specs=P(("sp", "tp"), None), check_vma=False
    )
```
